1024 devices in a mesh: kv: 128 (over z, y), tp: 8 (over x, core).
Axes of the slice: x: 4, y: 4, z: 32, core: 2. Of those that a mesh axis runs over, the one named last changes fastest.
Arguments:
- tokens: bfloat16 [16, 4096], P(None, 'kv')
- norm_gain: float32 [4096], P('kv'), may hold values from 0.1 to 1.9
- w_query: bfloat16 [4096, 3072], P('kv', 'tp'), may hold values from -0.09375 to 0.09375
- w_key: bfloat16 [4096, 3072], P('kv', 'tp'), may hold values from -0.09375 to 0.09375
- w_value: bfloat16 [4096, 3072], P('kv', 'tp'), may hold values from -0.09375 to 0.09375
- w_forget: bfloat16 [4096, 48], P('kv'), may hold values from -0.09375 to 0.09375
- w_out: bfloat16 [3072, 4096], P('tp', 'kv'), may hold values from -0.109375 to 0.109375
- mix_gain: float32 [4096], P('kv'), may hold values from 0.1 to 1.9
- w_up: bfloat16 [4096, 16384], P('kv', 'tp'), may hold values from -0.09375 to 0.09375
- w_down: bfloat16 [16384, 4096], P('tp', 'kv'), may hold values from -0.0625 to 0.0625
- key_cache: bfloat16 [16, 16384, 3072], P(None, 'kv', 'tp')
- value_cache: bfloat16 [16, 16384, 3072], P(None, 'kv', 'tp'), may hold values from -6 to 6
- decay_cache: float32 [16, 48, 16384], P(None, 'tp', 'kv')
- lengths: int32 [16], replicated, may hold values from 1 to 16384, 87381 in all
Outputs:
- layer_out: bfloat16 [16, 4096], P(None, 'kv')
The draws below stay inside these ranges and needn't reach their ends.
Inputs may be any that keep to these rules, and one draw needn't show every extreme that they name: `lengths`: one sequence fills all 16384 positions.
All inputs are finite; a program needn't handle non-finite values.
Results may differ from the reference program's by a relative error of at most 0.01.
Values may be sent and summed in bfloat16 or wider, within the bound.
No kernel may reach another device: no remote copies, remote signals or barrier semaphores. Data moves between devices by JAX's collectives and lax.ppermute only.
A program may use at most 64 MiB of HBM per device.

```python
import math
import jax
import jax.numpy as jnp
import numpy as np
from jax import lax

D = 4096
ATTENTION_HEADS = 48
HEAD_DIM = 64
FF = 16384
BATCH_SEQUENCES = 16
POS_DEV = 128
ATT = 3072
CACHE_CAPACITY = 16384


def draw_tokens(key, part):
    flow_lanes = jax.random.split(jax.random.fold_in(key, 3), 2)
    columns = jnp.arange(D, dtype=jnp.float32)
    column_scale = 10.0 ** (columns / D)
    row_factor = jnp.exp(jax.random.uniform(flow_lanes[0], (BATCH_SEQUENCES, 1), jnp.float32, 0.0, jnp.log(4.0)))
    sample = jax.random.normal(flow_lanes[1], (BATCH_SEQUENCES, D), jnp.float32)
    return (sample * column_scale * row_factor / 5.0).astype(jnp.bfloat16)


def draw_key_cache(key, part):
    flow_lanes = jax.random.split(jax.random.fold_in(key, 5), 1)
    sample = jax.random.normal(flow_lanes[0], (BATCH_SEQUENCES, CACHE_CAPACITY, ATT), jnp.float32)
    return sample.astype(jnp.bfloat16)


def draw_value_cache(key, part):
    flow_lanes = jax.random.split(jax.random.fold_in(key, 11), 3)
    block_count = CACHE_CAPACITY // POS_DEV
    channel_mean = jax.random.uniform(flow_lanes[0], (BATCH_SEQUENCES, 1, 1, ATT), jnp.float32, -2.0, 2.0)
    block_offset = jax.random.uniform(flow_lanes[1], (BATCH_SEQUENCES, block_count, 1, ATT), jnp.float32, -1.5, 1.5)
    noise = jax.random.normal(flow_lanes[2], (BATCH_SEQUENCES, block_count, POS_DEV, ATT), jnp.float32)
    sample = jnp.clip(channel_mean + block_offset + noise, -6.0, 6.0)
    return sample.reshape(BATCH_SEQUENCES, CACHE_CAPACITY, ATT).astype(jnp.bfloat16)


def draw_decay_cache(key, part):
    flow_lanes = jax.random.split(jax.random.fold_in(key, 7), 7)
    slow_share = 0.5
    gradual_heads = (jax.random.uniform(flow_lanes[0], (BATCH_SEQUENCES, ATTENTION_HEADS, 1), jnp.float32) < slow_share).astype(jnp.float32)
    slow_rate = jax.random.uniform(flow_lanes[1], (BATCH_SEQUENCES, ATTENTION_HEADS, 1), jnp.float32, 0.3, 0.8) / CACHE_CAPACITY
    fast_rate = jax.random.uniform(flow_lanes[2], (BATCH_SEQUENCES, ATTENTION_HEADS, 1), jnp.float32, 0.02, 0.035)
    decay_rates = gradual_heads * slow_rate + (1.0 - gradual_heads) * fast_rate
    block_count = CACHE_CAPACITY // POS_DEV
    block_multiplier = jnp.exp(jax.random.uniform(flow_lanes[3], (BATCH_SEQUENCES, ATTENTION_HEADS, block_count, 1), jnp.float32, jnp.log(0.4), jnp.log(2.5)))
    block_multiplier = jnp.broadcast_to(block_multiplier, (BATCH_SEQUENCES, ATTENTION_HEADS, block_count, POS_DEV)).reshape(BATCH_SEQUENCES, ATTENTION_HEADS, CACHE_CAPACITY)
    jaggedness = jax.random.uniform(flow_lanes[4], (BATCH_SEQUENCES, ATTENTION_HEADS, CACHE_CAPACITY), jnp.float32, 0.5, 1.5)
    spike_events = (jax.random.uniform(flow_lanes[5], (BATCH_SEQUENCES, ATTENTION_HEADS, CACHE_CAPACITY), jnp.float32) < 3.0 / CACHE_CAPACITY).astype(jnp.float32)
    spike_removal = jax.random.uniform(flow_lanes[6], (BATCH_SEQUENCES, ATTENTION_HEADS, CACHE_CAPACITY), jnp.float32, 0.22, 0.69)
    forget_gates = -decay_rates * block_multiplier * jaggedness - spike_events * spike_removal * gradual_heads
    return jnp.cumsum(forget_gates, axis=2)


def steps_of(stream_key, dims, cuts, smallest, largest):
    loudness = 1.0
    for dim, parts in cuts:
        heights = jax.random.uniform(jax.random.fold_in(jax.random.fold_in(stream_key, 6), dim), (parts,), jnp.float32, smallest / len(cuts), largest / len(cuts))
        loudness = loudness * jnp.repeat(jnp.exp(heights), dims[dim] // parts).reshape((-1,) + (1,) * (len(dims) - 1 - dim))
    return loudness


def split_up(number_of, total, limit, skew):
    loads = [(1 << 20) // math.isqrt(standing ** skew) + 1 for standing in range(2, number_of + 1)]
    spare, counts = total - limit - (number_of - 1), [1] * (number_of - 1)
    while spare > 0:
        movable = [i for i in range(number_of - 1) if counts[i] < limit]
        whole, left = sum([loads[i] for i in movable]), spare
        for i in movable:
            more = min(limit - counts[i], max(1, left * loads[i] // whole), spare)
            counts[i] = counts[i] + more
            spare = spare - more
    return np.array([limit] + counts)


def ragged_sizes(rng, number_of, total, limit, slope):
    if number_of == 2:
        one = jax.random.randint(rng, (), max(1, total - limit), min(limit, total - 1) + 1)
        return jnp.stack([one, total - one])
    sizes = jnp.asarray(split_up(number_of, total, limit, slope), jnp.int32)
    twos = (number_of - 1) // 2
    giver, receiver = sizes[1:1 + 2 * twos:2], sizes[2:2 + 2 * twos:2]
    margin = jnp.minimum(giver - 1, limit - receiver)
    shifted = jax.random.randint(jax.random.fold_in(rng, 1), (twos,), 0, 1 << 20) % (margin + 1)
    sizes = sizes.at[1:1 + 2 * twos:2].set(giver - shifted).at[2:2 + 2 * twos:2].set(receiver + shifted)
    return sizes[jax.random.permutation(jax.random.fold_in(rng, 2), number_of)]


def gaussian(stream_key, extent, deviation, limit, pieces=(), kind=jnp.bfloat16):
    gain = steps_of(stream_key, extent, pieces, -0.22, 0.18) if pieces else 1.0
    values = jax.random.normal(stream_key, extent, jnp.float32) * deviation * gain
    return jnp.minimum(jnp.maximum(values, -limit), limit).astype(kind)


def setup_inputs(seed: int = 0) -> dict:
    seeds = jax.random.split(jax.random.key(seed), 15)
    tokens = draw_tokens(jax.random.fold_in(seeds[14], 71), 0)
    norm_gain = jnp.clip(1.0 + 0.18 * jax.random.normal(seeds[1], (D,), jnp.float32), 0.1, 1.9)
    w_query = gaussian(seeds[2], (D, ATT), D ** -0.5, 0.09375, ((0, 128), (1, 8)))
    w_key = gaussian(seeds[3], (D, ATT), D ** -0.5, 0.09375, ((0, 128), (1, 8)))
    w_value = gaussian(seeds[4], (D, ATT), D ** -0.5, 0.09375, ((0, 128), (1, 8)))
    w_forget = gaussian(seeds[5], (D, ATTENTION_HEADS), D ** -0.5, 0.09375, ((0, 128),))
    w_out = gaussian(seeds[6], (ATT, D), ATT ** -0.5, 0.109375, ((0, 8), (1, 128)))
    mix_gain = jnp.clip(1.0 + 0.18 * jax.random.normal(seeds[7], (D,), jnp.float32), 0.1, 1.9)
    w_up = gaussian(seeds[8], (D, FF), D ** -0.5, 0.09375, ((0, 128), (1, 8)))
    w_down = gaussian(seeds[9], (FF, D), (FF // 2) ** -0.5, 0.0625, ((0, 8), (1, 128)))
    key_cache = draw_key_cache(jax.random.fold_in(seeds[14], 71), 0)
    value_cache = draw_value_cache(jax.random.fold_in(seeds[14], 71), 0)
    decay_cache = draw_decay_cache(jax.random.fold_in(seeds[14], 71), 0)
    lengths = ragged_sizes(seeds[13], BATCH_SEQUENCES, BATCH_SEQUENCES * CACHE_CAPACITY // 3, CACHE_CAPACITY, 2).astype(jnp.int32)
    return {"tokens": tokens, "norm_gain": norm_gain, "w_query": w_query, "w_key": w_key, "w_value": w_value, "w_forget": w_forget, "w_out": w_out, "mix_gain": mix_gain, "w_up": w_up, "w_down": w_down, "key_cache": key_cache, "value_cache": value_cache, "decay_cache": decay_cache, "lengths": lengths}


epsilon = 1e-06
very_low = -1e+30

def block_softmax(query_heads, score_bias, keys_block, values_block, live_mask):
    rows_count, count = (keys_block.shape[0], keys_block.shape[1])
    heads_count = query_heads.shape[1]
    keys_float = keys_block.astype(jnp.float32).reshape(rows_count, count, heads_count, HEAD_DIM)
    values_float = values_block.astype(jnp.float32).reshape(rows_count, count, heads_count, HEAD_DIM)
    scores = jnp.einsum('bhe,bphe->bhp', query_heads, keys_float) * HEAD_DIM ** (-0.5) + score_bias
    block_peak = lax.optimization_barrier(jnp.max(jnp.where(live_mask, scores, very_low), axis=2))
    weights = jnp.where(live_mask, jnp.exp(scores - block_peak[..., None]), 0.0)
    totals = lax.optimization_barrier(jnp.sum(weights, axis=2))
    rounded = lax.optimization_barrier(weights.astype(jnp.bfloat16)).astype(jnp.float32)
    weighted = jnp.einsum('bhp,bphe->bhe', rounded, values_float)
    return (block_peak, totals, weighted)

def join(earlier, later_part):
    highest = jnp.maximum(earlier[0], later_part[0])
    factor_one = jnp.exp(earlier[0] - highest)
    factor_two = jnp.exp(later_part[0] - highest)
    totals = earlier[1] * factor_one + later_part[1] * factor_two
    weighted = earlier[2] * factor_one[..., None] + later_part[2] * factor_two[..., None]
    return (highest, totals, weighted)

def reference(tokens, norm_gain, w_query, w_key, w_value, w_forget, w_out, mix_gain, w_up, w_down, key_cache, value_cache, decay_cache, lengths):
    rows_count = tokens.shape[0]
    tokens_f = tokens.astype(jnp.float32)
    row_scale = lax.rsqrt(lax.optimization_barrier(jnp.mean(tokens_f * tokens_f, axis=1)) + epsilon)[:, None]
    scaled_in = (tokens_f * norm_gain.astype(jnp.float32)).astype(jnp.bfloat16)
    queries = (row_scale * jnp.dot(scaled_in, w_query, preferred_element_type=jnp.float32)).astype(jnp.bfloat16)
    new_keys = (row_scale * jnp.dot(scaled_in, w_key, preferred_element_type=jnp.float32)).astype(jnp.bfloat16)
    new_values = (row_scale * jnp.dot(scaled_in, w_value, preferred_element_type=jnp.float32)).astype(jnp.bfloat16)
    log_forget = jax.nn.log_sigmoid(row_scale * jnp.dot(scaled_in, w_forget, preferred_element_type=jnp.float32))
    positions = jnp.arange(CACHE_CAPACITY, dtype=jnp.int32)
    newest = positions[None, None, :] == (lengths - 1)[:, None, None]
    now_decay = lax.optimization_barrier(jnp.sum(jnp.where(newest, decay_cache, 0.0), axis=2)) + log_forget
    query_heads = queries.astype(jnp.float32).reshape(rows_count, ATTENTION_HEADS, HEAD_DIM)
    own_keys = new_keys.astype(jnp.float32).reshape(rows_count, ATTENTION_HEADS, HEAD_DIM)
    own_score = lax.optimization_barrier(jnp.sum(query_heads * own_keys, axis=2)) * HEAD_DIM ** (-0.5)
    start_state = (own_score, jnp.ones_like(own_score), new_values.astype(jnp.float32).reshape(rows_count, ATTENTION_HEADS, HEAD_DIM))

    def visit(carried, block_index):
        offset = block_index * POS_DEV
        keys_block = lax.dynamic_slice_in_dim(key_cache, offset, POS_DEV, 1)
        values_block = lax.dynamic_slice_in_dim(value_cache, offset, POS_DEV, 1)
        decay_block = lax.dynamic_slice_in_dim(decay_cache, offset, POS_DEV, 2)
        live_mask = (offset + jnp.arange(POS_DEV, dtype=jnp.int32))[None, None, :] < lengths[:, None, None]
        piece_state = block_softmax(query_heads, now_decay[:, :, None] - decay_block, keys_block, values_block, live_mask)
        return (join(carried, piece_state), None)
    final_state, unused = lax.scan(visit, start_state, jnp.arange(CACHE_CAPACITY // POS_DEV, dtype=jnp.int32))
    attended = (final_state[2] / final_state[1][..., None]).reshape(rows_count, ATTENTION_HEADS * HEAD_DIM).astype(jnp.bfloat16)
    mixed_in = (tokens_f + jnp.dot(attended, w_out, preferred_element_type=jnp.float32)).astype(jnp.bfloat16)
    mixed_f = mixed_in.astype(jnp.float32)
    mix_scale = lax.rsqrt(lax.optimization_barrier(jnp.mean(mixed_f * mixed_f, axis=1)) + epsilon)[:, None]
    mix_in = (mixed_f * mix_gain.astype(jnp.float32)).astype(jnp.bfloat16)
    upward = mix_scale * jnp.dot(mix_in, w_up, preferred_element_type=jnp.float32)
    hidden = (jax.nn.relu(upward) ** 2).astype(jnp.bfloat16)
    return (mixed_f + jnp.dot(hidden, w_down, preferred_element_type=jnp.float32)).astype(jnp.bfloat16)
```

```python
import jax
import jax.numpy as jnp
from jax import lax
from jax.experimental import pallas as pl
from jax.experimental.pallas import tpu as pltpu
from jax.sharding import Mesh
from jax.sharding import PartitionSpec as P

HEAD_DIM = 64
LANES = 128
KV = ("kv_0", "kv_1")
epsilon = 1e-06
very_low = -1e30
f32 = jnp.float32
bf16 = jnp.bfloat16

VMEM = pl.BlockSpec(memory_space=pltpu.VMEM)
SMEM = pl.BlockSpec(memory_space=pltpu.SMEM)
NT = (((1,), (1,)), ((), ()))


def exchanged(x, axes):
    return lax.all_to_all(x, axes, 0, 0, tiled=True)


def lane_of(shape):
    return lax.broadcasted_iota(jnp.int32, shape, len(shape) - 1)


def split_in_three(x):
    high = lax.reduce_precision(x, 8, 7)
    rest = x - high
    middle = lax.reduce_precision(rest, 8, 7)
    return high, middle, rest - middle


def length_column(lengths_ref, rows, width):
    row = lax.broadcasted_iota(jnp.int32, (rows, width), 0)
    out = jnp.zeros((rows, width), jnp.int32)
    for b in range(rows):
        out = jnp.where(row == b, lengths_ref[b], out)
    return out


def first_position(span):
    return (lax.axis_index("kv_0") * lax.axis_size("kv_1") + lax.axis_index("kv_1")) * span


def project_kernel(tokens, gain, w_query, w_key, w_value, w_forget, decay, lengths, out):
    rows = tokens.shape[0]
    heads = decay.shape[0]
    span = decay.shape[2]
    slots = out.shape[0] // rows
    x = tokens[...].astype(f32)
    scaled = (x * gain[...]).astype(bf16)
    q = jnp.dot(scaled, w_query[...], preferred_element_type=f32)
    k = jnp.dot(scaled, w_key[...], preferred_element_type=f32)
    v = jnp.dot(scaled, w_value[...], preferred_element_type=f32)
    gates = jnp.dot(scaled, w_forget[...], preferred_element_type=f32)
    squares = jnp.sum(x * x, axis=1, keepdims=True)
    position = first_position(span) + lane_of((rows, span))
    newest = position == length_column(lengths, rows, span) - 1
    gate_lane = lane_of(gates.shape)
    lane = lane_of((rows, HEAD_DIM))
    first_head = lax.axis_index("tp") * heads
    for h in range(slots):
        if h < heads:
            cols = slice(h * HEAD_DIM, (h + 1) * HEAD_DIM)
            gate = jnp.sum(jnp.where(gate_lane == first_head + h, gates, 0.0), axis=1, keepdims=True)
            last = jnp.sum(jnp.where(newest, decay[h], 0.0), axis=1, keepdims=True)
            high, middle, low = split_in_three(last)
            extra = jnp.where(lane == 0, gate, 0.0)
            extra = jnp.where(lane == 1, high, extra)
            extra = jnp.where(lane == 2, middle, extra)
            extra = jnp.where(lane == 3, low, extra)
            extra = jnp.where(lane == 4, squares, extra)
            top = jnp.concatenate([q[:, cols], k[:, cols]], axis=1)
            bottom = jnp.concatenate([v[:, cols], extra], axis=1)
        else:
            top = bottom = jnp.zeros((rows, LANES), f32)
        for b in range(rows):
            both = jnp.concatenate([top[b : b + 1], bottom[b : b + 1]], axis=0)
            out[b * slots + h] = both.astype(bf16)


def query_kernel(width, got, out, state):
    total = jnp.sum(got[...].astype(f32), axis=0)
    top, bottom = total[0:1], total[1:2]
    lane = lane_of((1, LANES))
    pick = lambda i: jnp.sum(jnp.where(lane == HEAD_DIM + i, bottom, 0.0), axis=1, keepdims=True)
    row_scale = lax.rsqrt(pick(4) / width + epsilon)
    top = (row_scale * top).astype(bf16).astype(f32)
    value = (row_scale * bottom).astype(bf16).astype(f32)
    own = (
        jnp.sum(top[:, :HEAD_DIM] * top[:, HEAD_DIM:], axis=1, keepdims=True) * HEAD_DIM ** (-0.5)
    )
    gate = row_scale * pick(0)
    log_forget = jnp.minimum(gate, 0.0) - jnp.log1p(jnp.exp(-jnp.abs(gate)))
    now_decay = pick(1) + pick(2) + pick(3) + log_forget
    out[...] = jnp.broadcast_to(top[None], out.shape)
    row = jnp.where(lane == HEAD_DIM, own, value)
    row = jnp.where(lane == HEAD_DIM + 1, now_decay, row)
    state[...] = jnp.broadcast_to(row, state.shape)


def attend_kernel(queries, keys, values, decay, lengths, out):
    rows, slots, _ = queries.shape
    heads = decay.shape[0]
    span = keys.shape[1]
    channels = keys.shape[2]
    position = first_position(span) + lane_of((slots, span))
    mine = lane_of((slots, channels)) // HEAD_DIM == lax.broadcasted_iota(
        jnp.int32, (slots, channels), 0
    )
    lane = lane_of((slots, HEAD_DIM))
    for b in range(rows):
        q = queries[b][:, :HEAD_DIM] * HEAD_DIM ** (-0.5)
        q = jnp.concatenate([q] * heads, axis=1)
        q = jnp.where(mine, q, 0.0).astype(bf16)
        scores = lax.dot_general(q, keys[b], NT, preferred_element_type=f32)
        parts = [decay[h, b : b + 1, :] for h in range(heads)]
        if slots > heads:
            parts.append(jnp.zeros((slots - heads, span), f32))
        scores = scores - jnp.concatenate(parts, axis=0)
        live = position < lengths[b]
        peak = jnp.max(jnp.where(live, scores, very_low), axis=1, keepdims=True)
        weights = jnp.where(live, jnp.exp(scores - peak), 0.0)
        total = jnp.sum(weights, axis=1, keepdims=True)
        mixed = jnp.dot(weights.astype(bf16), values[b], preferred_element_type=f32)
        mixed = jnp.where(mine, mixed, 0.0)
        folded = mixed[:, :HEAD_DIM]
        for h in range(1, heads):
            folded = folded + mixed[:, h * HEAD_DIM : (h + 1) * HEAD_DIM]
        tail = jnp.where(lane == 0, peak, jnp.where(lane == 1, total, 0.0))
        out[b] = jnp.concatenate([folded, tail], axis=1)


def combine_kernel(got, state, out):
    rows, slots, _ = got.shape
    r = got[...].reshape(rows * slots, LANES)
    row = state[0:1]
    lane = lane_of((1, LANES))
    own = jnp.sum(jnp.where(lane == HEAD_DIM, row, 0.0), axis=1, keepdims=True)
    now_decay = jnp.sum(jnp.where(lane == HEAD_DIM + 1, row, 0.0), axis=1, keepdims=True)
    peaks = r[:, HEAD_DIM : HEAD_DIM + 1] + now_decay
    peak = jnp.maximum(jnp.max(peaks, axis=0, keepdims=True), own)
    acc = jnp.sum(jnp.exp(peaks - peak) * r, axis=0, keepdims=True)
    mine = jnp.exp(own - peak)
    total = jnp.sum(jnp.where(lane == HEAD_DIM + 1, acc, 0.0), axis=1, keepdims=True) + mine
    attended = (acc + mine * row) / total
    attended = attended.astype(bf16).astype(f32)
    out[...] = jnp.broadcast_to(attended[None], out.shape)


def output_kernel(heads, got, block, out, aside):
    attended = jnp.concatenate([got[:, h, :][:, :HEAD_DIM] for h in range(heads)], axis=1)
    channels = heads * HEAD_DIM
    terms = lax.dot_general(
        attended.astype(bf16), block[:, :channels], NT, preferred_element_type=f32
    ).astype(bf16)
    for i in range(out.shape[0]):
        out[i] = terms
    turned = block[:, channels:].astype(f32).T
    aside[...] = turned[: aside.shape[0]]


def up_kernel(got, aside, w_up, out, mixed_out):
    rows = got.shape[1]
    terms = got[0].astype(f32)
    for i in range(1, got.shape[0]):
        terms = terms + got[i].astype(f32)
    gain = aside[rows : rows + 1] + aside[rows + 1 : rows + 2] + aside[rows + 2 : rows + 3]
    mixed = (aside[:rows] + terms).astype(bf16)
    mixed_out[...] = mixed
    mixed = mixed.astype(f32)
    squares = jnp.sum(mixed * mixed, axis=1, keepdims=True)
    high, middle, low = split_in_three(squares)
    up = jnp.dot((mixed * gain).astype(bf16), w_up[...], preferred_element_type=f32).astype(bf16)
    lane = lane_of((rows, LANES))
    tail = jnp.where(lane == 0, high, jnp.where(lane == 1, middle, jnp.where(lane == 2, low, 0.0)))
    tail = tail.astype(bf16)
    hidden = up.shape[1]
    for i in range(out.shape[0]):
        out[i, :, :hidden] = up
        out[i, :, hidden:] = tail


def down_kernel(width, got, w_down, out):
    hidden = w_down.shape[1]
    total = got[0].astype(f32)
    for i in range(1, got.shape[0]):
        total = total + got[i].astype(f32)
    squares = jnp.sum(total[:, hidden:], axis=1, keepdims=True)
    mix_scale = lax.rsqrt(squares / width + epsilon)
    live = jnp.maximum(mix_scale * total[:, :hidden], 0.0)
    terms = lax.dot_general(
        (live * live).astype(bf16), w_down[...], NT, preferred_element_type=f32
    )
    rows, columns = terms.shape
    terms = jnp.concatenate([terms, jnp.zeros((rows, LANES - columns), f32)], axis=1)
    for i in range(out.shape[0]):
        out[i] = terms


def room(mebibytes):
    return pltpu.CompilerParams(vmem_limit_bytes=mebibytes << 20)


def call(kernel, outs, *args, specs=None, mebibytes=8):
    return pl.pallas_call(
        kernel,
        out_shape=outs,
        compiler_params=room(mebibytes),
        in_specs=specs or [VMEM] * len(args),
        out_specs=jax.tree.map(lambda _: VMEM, outs),
    )(*args)


def shaped(shape, dtype):
    return jax.ShapeDtypeStruct(shape, dtype)


def shards(
    tokens,
    norm_gain,
    w_query,
    w_key,
    w_value,
    w_forget,
    w_out,
    mix_gain,
    w_up,
    w_down,
    key_cache,
    value_cache,
    decay_cache,
    lengths,
):
    rows, features = tokens.shape
    devices = lax.axis_size(KV)
    far = lax.axis_size("kv_0")
    near = lax.axis_size("kv_1")
    groups = lax.axis_size("tp")
    width = features * devices
    heads = decay_cache.shape[1]
    slots = devices // rows
    hidden = w_up.shape[1]
    decay = jnp.transpose(decay_cache, (1, 0, 2))
    gain_parts = jnp.stack(split_in_three(mix_gain)).astype(bf16)
    aside = jnp.concatenate([tokens, gain_parts], axis=0).T
    aside = jnp.pad(aside, ((0, 0), (0, LANES - aside.shape[1])))
    bundle = jnp.concatenate([w_up, w_out.T, aside], axis=1)
    gathered = lax.all_gather(bundle, "kv_0", tiled=True)
    side = bundle.shape[1] - hidden
    deep = gathered.shape[0]

    pieces = call(
        project_kernel,
        shaped((devices, 2, LANES), bf16),
        tokens,
        norm_gain[None],
        w_query,
        w_key,
        w_value,
        w_forget,
        decay,
        lengths,
        specs=[VMEM] * 7 + [SMEM],
    )
    got = exchanged(pieces, KV)
    spread, state = call(
        lambda *refs: query_kernel(width, *refs),
        (shaped((rows, slots, LANES), f32), shaped((8, LANES), f32)),
        got,
    )
    got = exchanged(spread.reshape(devices, 1, LANES), KV).reshape(rows, slots, LANES)
    local = call(
        attend_kernel,
        shaped((rows, slots, LANES), f32),
        got,
        key_cache,
        value_cache,
        decay,
        lengths,
        specs=[VMEM] * 4 + [SMEM],
    )
    got = exchanged(local.reshape(devices, 1, LANES), KV).reshape(rows, slots, LANES)
    spread = call(combine_kernel, shaped((rows, slots, LANES), f32), got, state)
    got = exchanged(spread.reshape(devices, 1, LANES), KV).reshape(rows, slots, LANES)
    whole = lambda shape: pl.BlockSpec(shape, lambda i: (0,) * len(shape))
    terms, aside = pl.pallas_call(
        lambda *refs: output_kernel(heads, *refs),
        grid=(1,),
        compiler_params=room(8),
        out_shape=(shaped((groups, rows, deep), bf16), shaped((rows + 8, deep), f32)),
        in_specs=[whole(got.shape), pl.BlockSpec((deep, side), lambda i: (0, hidden // side))],
        out_specs=(whole((groups, rows, deep)), whole((rows + 8, deep))),
    )(got, gathered)
    got = exchanged(terms, "tp")
    up, mixed = pl.pallas_call(
        up_kernel,
        grid=(1,),
        compiler_params=room(16),
        out_shape=(shaped((near, rows, hidden + LANES), bf16), shaped((rows, deep), bf16)),
        in_specs=[
            whole(got.shape),
            whole(aside.shape),
            pl.BlockSpec((deep, hidden), lambda i: (0, 0)),
        ],
        out_specs=(whole((near, rows, hidden + LANES)), whole((rows, deep))),
    )(got, aside, gathered)
    got = exchanged(up, "kv_1")
    down = call(
        lambda *refs: down_kernel(width, *refs),
        shaped((groups, rows, LANES), f32),
        got,
        w_down.T,
    )
    got = exchanged(down, "tp")
    mine = lax.dynamic_slice_in_dim(mixed, lax.axis_index("kv_0") * features, features, 1)
    total = jnp.sum(got, axis=0)[:, :features]
    return (mine.astype(f32) + total).astype(bf16)


def solution(mesh):
    near = 4
    far = mesh.shape["kv"] // near
    torus = Mesh(
        mesh.devices.reshape(far, near, mesh.shape["tp"]), ("kv_0", "kv_1", "tp")
    )
    placed = (
        P(None, KV),
        P(KV),
        P(KV, "tp"),
        P(KV, "tp"),
        P(KV, "tp"),
        P(KV, None),
        P("tp", KV),
        P(KV),
        P(KV, "tp"),
        P("tp", KV),
        P(None, KV, "tp"),
        P(None, KV, "tp"),
        P(None, "tp", KV),
        P(),
    )
    return jax.shard_map(
        shards, mesh=torus, in_specs=placed, out_specs=P(None, KV), check_vma=False
    )
```
